512 devices in a mesh: ra: 16 (over y, x), cb: 32 (over z, core).
Axes of the slice: x: 4, y: 4, z: 16, core: 2. Of those that a mesh axis runs over, the one named last changes fastest.
Arguments:
- tokens: bfloat16 [8192, 2048], P('cb', 'ra'), may hold values from -40 to 40
- gain_first: float32 [2048], replicated, may hold values from 0.1 to 1.9
- gate_first: float32 [2048, 5632], P('cb', 'ra'), may hold values from -0.125 to 0.125
- gate_first_scale: float32 [5632], P('ra'), may hold values from 0.5 to 2
- up_first: float32 [2048, 5632], P('cb', 'ra'), may hold values from -0.125 to 0.125
- up_first_scale: float32 [5632], P('ra'), may hold values from 0.5 to 2
- down_first: float32 [5632, 2048], P('ra', 'cb'), may hold values from -0.078125 to 0.078125
- down_first_scale: float32 [2048], replicated, may hold values from 0.5 to 2
- gain_second: float32 [2048], replicated, may hold values from 0.1 to 1.9
- gate_second: float32 [2048, 5632], P('cb', 'ra'), may hold values from -0.125 to 0.125
- gate_second_scale: float32 [5632], P('ra'), may hold values from 0.5 to 2
- up_second: float32 [2048, 5632], P('cb', 'ra'), may hold values from -0.125 to 0.125
- up_second_scale: float32 [5632], P('ra'), may hold values from 0.5 to 2
- down_second: float32 [5632, 2048], P('ra', 'cb'), may hold values from -0.078125 to 0.078125
- down_second_scale: float32 [2048], replicated, may hold values from 0.5 to 2
- gain_last: float32 [2048], replicated, may hold values from 0.1 to 1.9
Outputs:
- mixed: bfloat16 [8192, 2048], P('cb', 'ra')
The draws below stay inside these ranges and needn't reach their ends.
All inputs are finite; a program needn't handle non-finite values.
Results may differ from the reference program's by a relative error of at most 0.025.
Values may be sent and summed in bfloat16 or wider, within the bound.
No kernel may reach another device: no remote copies, remote signals or barrier semaphores. Data moves between devices by JAX's collectives and lax.ppermute only.
A program may use at most 64 MiB of HBM per device.

```python
import math
import jax
import jax.numpy as jnp
from jax import lax

D = 2048
FF = 5632
TOK = 8192


def draw_tokens(key, part):
    first_key = jax.random.fold_in(key, 11)
    second_key = jax.random.fold_in(key, 12)
    column = jnp.arange(D, dtype=jnp.float32)
    rising = 10.0 ** (column / D) * jax.random.uniform(first_key, (D,), jnp.float32, 0.6, 1.6)
    values = jnp.clip(jax.random.normal(second_key, (TOK, D), jnp.float32), -4.0, 4.0)
    return jnp.clip(values * rising, -40.0, 40.0).astype(jnp.bfloat16)


def levels(key, extent, shards, least, high):
    loudness, own = 1.0, jax.random.fold_in(key, 6)
    for axis_at, blocks in shards:
        heights = jnp.exp(jax.random.uniform(jax.random.fold_in(own, axis_at), (blocks,), jnp.float32, least / len(shards), high / len(shards)))
        loudness = loudness * jnp.repeat(heights, extent[axis_at] // blocks).reshape([-1 if axis == axis_at else 1 for axis in range(len(extent))])
    return loudness


def centred(key, extent, scale, reach, pieces=(), kind=jnp.bfloat16):
    result = scale * jax.random.normal(key, extent, jnp.float32)
    if pieces:
        result = result * levels(key, extent, pieces, -0.22, 0.18)
    return jnp.clip(result, -reach, reach).astype(kind)


def setup_inputs(seed: int = 0) -> dict:
    keys = jax.random.split(jax.random.key(seed), 17)
    tokens = draw_tokens(jax.random.fold_in(keys[16], 71), 0)
    gain_first = jnp.clip(1.0 + 0.18 * jax.random.normal(keys[1], (D,), jnp.float32), 0.1, 1.9)
    gate_first = centred(keys[2], (D, FF), D ** -0.5, 0.125, ((0, 32), (1, 16)), jnp.float32)
    gate_first_scale = jnp.clip(jnp.exp(math.log(2.0) - 1.3862944 * jax.random.uniform(keys[3], (FF,), jnp.float32) ** levels(keys[3], (FF,), ((0, 16),), -0.2, 0.2)), 0.5, 2.0)
    up_first = centred(keys[4], (D, FF), D ** -0.5, 0.125, ((0, 32), (1, 16)), jnp.float32)
    up_first_scale = jnp.clip(jnp.exp(math.log(2.0) - 1.3862944 * jax.random.uniform(keys[5], (FF,), jnp.float32) ** levels(keys[5], (FF,), ((0, 16),), -0.2, 0.2)), 0.5, 2.0)
    down_first = centred(keys[6], (FF, D), FF ** -0.5, 0.078125, ((0, 16), (1, 32)), jnp.float32)
    down_first_scale = jnp.clip(jnp.exp(jax.random.uniform(keys[7], (D,), jnp.float32, math.log(0.5), math.log(2.0))), 0.5, 2.0)
    gain_second = jnp.clip(1.0 + 0.18 * jax.random.normal(keys[8], (D,), jnp.float32), 0.1, 1.9)
    gate_second = centred(keys[9], (D, FF), D ** -0.5, 0.125, ((0, 32), (1, 16)), jnp.float32)
    gate_second_scale = jnp.clip(jnp.exp(math.log(2.0) - 1.3862944 * jax.random.uniform(keys[10], (FF,), jnp.float32) ** levels(keys[10], (FF,), ((0, 16),), -0.2, 0.2)), 0.5, 2.0)
    up_second = centred(keys[11], (D, FF), D ** -0.5, 0.125, ((0, 32), (1, 16)), jnp.float32)
    up_second_scale = jnp.clip(jnp.exp(math.log(2.0) - 1.3862944 * jax.random.uniform(keys[12], (FF,), jnp.float32) ** levels(keys[12], (FF,), ((0, 16),), -0.2, 0.2)), 0.5, 2.0)
    down_second = centred(keys[13], (FF, D), FF ** -0.5, 0.078125, ((0, 16), (1, 32)), jnp.float32)
    down_second_scale = jnp.clip(jnp.exp(jax.random.uniform(keys[14], (D,), jnp.float32, math.log(0.5), math.log(2.0))), 0.5, 2.0)
    gain_last = jnp.clip(1.0 + 0.18 * jax.random.normal(keys[15], (D,), jnp.float32), 0.1, 1.9)
    return dict(tokens=tokens, gain_first=gain_first, gate_first=gate_first, gate_first_scale=gate_first_scale, up_first=up_first, up_first_scale=up_first_scale, down_first=down_first, down_first_scale=down_first_scale, gain_second=gain_second, gate_second=gate_second, gate_second_scale=gate_second_scale, up_second=up_second, up_second_scale=up_second_scale, down_second=down_second, down_second_scale=down_second_scale, gain_last=gain_last)


def gated_block(values, gain, w_gate, s_gate, w_up, s_up, w_down, s_down):
    meansq = lax.optimization_barrier(jnp.mean(values * values, axis=1, keepdims=True))
    normed = (values * lax.rsqrt(meansq + 1e-06) * gain).astype(jnp.bfloat16)
    gate = jnp.dot(normed, w_gate.astype(jnp.bfloat16), preferred_element_type=jnp.float32) * s_gate
    upper = jnp.dot(normed, w_up.astype(jnp.bfloat16), preferred_element_type=jnp.float32) * s_up
    hidden = (jax.nn.silu(gate) * upper).astype(jnp.bfloat16)
    return jnp.dot(hidden, w_down.astype(jnp.bfloat16), preferred_element_type=jnp.float32) * s_down

def reference(tokens, gain_first, gate_first, gate_first_scale, up_first, up_first_scale, down_first, down_first_scale, gain_second, gate_second, gate_second_scale, up_second, up_second_scale, down_second, down_second_scale, gain_last):
    start = tokens.astype(jnp.float32)
    first = 0.1 * start + 0.5 * gated_block(start, gain_first, gate_first, gate_first_scale, up_first, up_first_scale, down_first, down_first_scale)
    second = 0.1 * first + 0.5 * gated_block(first, gain_second, gate_second, gate_second_scale, up_second, up_second_scale, down_second, down_second_scale)
    meansq = lax.optimization_barrier(jnp.mean(second * second, axis=1, keepdims=True))
    return (second * lax.rsqrt(meansq + 1e-06) * gain_last).astype(jnp.bfloat16)
```

```python
import functools

import jax
import jax.numpy as jnp
from jax import lax
from jax.experimental import pallas as pl
from jax.experimental.pallas import tpu as pltpu
from jax.sharding import Mesh
from jax.sharding import PartitionSpec as P

D = 2048
RA = ("ra_0", "ra_1")
CB = ("cb_0", "cb_1")
LANES = 384
EPS = 1e-06


def pack_body(g1, u1, d1, g2, u2, d2, out):
    rows, width = g1.shape

    def put(at, value):
        out[:, at : at + LANES] = jnp.zeros((rows, LANES), jnp.bfloat16)
        out[:, at : at + width] = value.astype(jnp.bfloat16)

    put(0, g1[...])
    put(LANES, u1[...])
    put(2 * LANES, g2[...])
    put(3 * LANES, u2[...])
    put(4 * LANES, d1[...].T)
    put(5 * LANES, d2[...].T)


def pack(g1, u1, d1, g2, u2, d2):
    rows = g1.shape[0]
    return pl.pallas_call(
        pack_body,
        out_shape=jax.ShapeDtypeStruct((rows, 6 * LANES), jnp.bfloat16),
    )(g1, u1, d1, g2, u2, d2)


def block_body(steps, first, x, gain, w_in, w_down, s_gate, s_up, out, normed, gate_up, hidden):
    k = pl.program_id(0)
    chunk = w_in.shape[0]

    @pl.when(k == 0)
    def _():
        gate_up[...] = jnp.zeros_like(gate_up)
        if first:
            count = x.shape[0]
            total = jnp.zeros((x.shape[1], 1), jnp.float32)
            for j in range(count):
                piece = x[j].astype(jnp.float32)
                total += jnp.sum(piece * piece, axis=1, keepdims=True)
            scale = lax.rsqrt(total / D + EPS)
            for j in range(count):
                at = slice(j * x.shape[2], (j + 1) * x.shape[2])
                value = x[j].astype(jnp.float32) * scale * gain[:, at]
                normed[:, at] = value.astype(jnp.bfloat16)

    source = normed if first else x

    @pl.when(k < steps)
    def _():
        at = pl.multiple_of(k * chunk, chunk)
        gate_up[...] += jnp.dot(
            source[:, pl.ds(at, chunk)], w_in[...], preferred_element_type=jnp.float32
        )

    @pl.when(k == steps - 1)
    def _():
        gate = gate_up[:, :LANES] * s_gate[...]
        upper = gate_up[:, LANES:] * s_up[...]
        hidden[...] = (gate / (1.0 + jnp.exp(-gate)) * upper).astype(jnp.bfloat16)

    @pl.when(k >= steps)
    def _():
        out[...] = lax.dot_general(
            hidden[...],
            w_down[...],
            (((1,), (1,)), ((), ())),
            preferred_element_type=jnp.float32,
        ).astype(jnp.bfloat16)


def block(x, gain, weights, which, s_gate, s_up, steps=4):
    first = x.ndim == 3
    rows = x.shape[1] if first else x.shape[0]
    chunk = D // steps
    return pl.pallas_call(
        functools.partial(block_body, steps, first),
        grid=(2 * steps,),
        in_specs=[
            pl.BlockSpec(x.shape, lambda k: (0,) * x.ndim),
            pl.BlockSpec((1, D), lambda k: (0, 0)),
            pl.BlockSpec((chunk, 2 * LANES), lambda k: (jnp.minimum(k, steps - 1), which)),
            pl.BlockSpec((chunk, LANES), lambda k: (jnp.maximum(k - steps, 0), 4 + which)),
            pl.BlockSpec((1, LANES), lambda k: (0, 0)),
            pl.BlockSpec((1, LANES), lambda k: (0, 0)),
        ],
        out_specs=pl.BlockSpec((rows, chunk), lambda k: (0, jnp.maximum(k - steps, 0))),
        out_shape=jax.ShapeDtypeStruct((rows, D), jnp.bfloat16),
        scratch_shapes=[
            pltpu.VMEM((rows, D) if first else (8, 128), jnp.bfloat16),
            pltpu.VMEM((rows, 2 * LANES), jnp.float32),
            pltpu.VMEM((rows, LANES), jnp.bfloat16),
        ],
    )(x, gain, weights, weights, s_gate, s_up)


def exchange(pieces):
    return lax.all_to_all(pieces, RA, split_axis=0, concat_axis=0, tiled=True)


def copy_for_each(x):
    return exchange(jnp.broadcast_to(x, (lax.axis_size(RA), *x.shape)))


def by_rows(partial_value):
    pieces = partial_value.reshape(lax.axis_size(RA), -1, D)
    return exchange(pieces).astype(jnp.float32).sum(axis=0)


def normalized(values, gain):
    meansq = jnp.mean(values * values, axis=1, keepdims=True)
    return (values * lax.rsqrt(meansq + EPS) * gain).astype(jnp.bfloat16)


def padded(scale):
    return jnp.pad(scale, (0, LANES - scale.shape[0]))[None]


def shards(
    tokens,
    gain_first,
    gate_first,
    gate_first_scale,
    up_first,
    up_first_scale,
    down_first,
    down_first_scale,
    gain_second,
    gate_second,
    gate_second_scale,
    up_second,
    up_second_scale,
    down_second,
    down_second_scale,
    gain_last,
):
    count = lax.axis_size(RA)
    packed = pack(gate_first, up_first, down_first, gate_second, up_second, down_second)
    weights = lax.all_gather(packed, CB, axis=0, tiled=True)
    pieces = copy_for_each(tokens)
    rows = tokens.shape[0] // count
    own = lax.dynamic_slice_in_dim(pieces, lax.axis_index(RA) * rows, rows, 1)
    own = jnp.moveaxis(own, 0, 1).reshape(rows, D).astype(jnp.float32)
    partial_first = block(
        pieces, gain_first[None], weights, 0, padded(gate_first_scale), padded(up_first_scale)
    )
    first = 0.1 * own + 0.5 * by_rows(partial_first) * down_first_scale
    normed = copy_for_each(normalized(first, gain_second)).reshape(-1, D)
    partial_second = block(
        normed, gain_second[None], weights, 1, padded(gate_second_scale), padded(up_second_scale)
    )
    second = 0.1 * first + 0.5 * by_rows(partial_second) * down_second_scale
    mixed = normalized(second, gain_last)
    columns = jnp.moveaxis(mixed.reshape(rows, count, -1), 1, 0)
    return exchange(columns).reshape(tokens.shape)


def solution(mesh):
    torus = Mesh(mesh.devices.reshape(4, 4, 16, 2), ("ra_0", "ra_1", "cb_0", "cb_1"))
    weight, across = P(CB, RA), P(RA, CB)
    return jax.shard_map(
        shards,
        mesh=torus,
        in_specs=(
            P(CB, RA),
            P(),
            weight,
            P(RA),
            weight,
            P(RA),
            across,
            P(),
            P(),
            weight,
            P(RA),
            weight,
            P(RA),
            across,
            P(),
            P(),
        ),
        out_specs=P(CB, RA),
        check_vma=False,
    )
```

```python
import functools

import jax
import jax.numpy as jnp
from jax import lax
from jax.experimental import pallas as pl
from jax.experimental.pallas import tpu as pltpu
from jax.sharding import Mesh
from jax.sharding import PartitionSpec as P

D = 2048
RA = ("ra_0", "ra_1")
CB = ("cb_0", "cb_1")
LANES = 384
EPS = 1e-06
LIFT = 2.0**18
ROOM = pltpu.CompilerParams(vmem_limit_bytes=20 * 1024 * 1024)


def pack_body(g1, u1, d1, g2, u2, d2, out):
    rows, width = g1.shape
    out[...] = jnp.zeros_like(out)
    for j, piece in enumerate((g1, u1, d1, g2, u2, d2)):
        out[:, j * LANES : j * LANES + width] = piece[...].astype(jnp.bfloat16) * LIFT


def pack(g1, u1, d1, g2, u2, d2):
    rows = g1.shape[0]
    return pl.pallas_call(
        pack_body,
        out_shape=jax.ShapeDtypeStruct((rows, 6 * LANES), jnp.bfloat16),
        compiler_params=ROOM,
    )(g1, u1, d1.T, g2, u2, d2.T)


def spread_body(pieces, gain, out):
    count, rows, width = pieces.shape
    total = jnp.zeros((rows, 1), jnp.float32)
    for j in range(count):
        piece = pieces[j].astype(jnp.float32)
        total += jnp.sum(piece * piece, axis=1, keepdims=True)
    scale = lax.rsqrt(total / D + EPS)
    for j in range(count):
        at = slice(j * width, (j + 1) * width)
        out[:, at] = (pieces[j].astype(jnp.float32) * scale * gain[:, at]).astype(jnp.bfloat16)


def spread(pieces, gain):
    return pl.pallas_call(
        spread_body,
        out_shape=jax.ShapeDtypeStruct((pieces.shape[1], D), jnp.bfloat16),
        compiler_params=ROOM,
    )(pieces, gain[None])


def block_body(x, weights, s_gate, s_up, out):
    both = jnp.dot(x[...], weights[:, : 2 * LANES], preferred_element_type=jnp.float32)
    gate = both[:, :LANES] * s_gate[...]
    upper = both[:, LANES:] * s_up[...]
    hidden = (gate / (1.0 + jnp.exp(-gate)) * upper).astype(jnp.bfloat16)
    out[...] = lax.dot_general(
        hidden,
        weights[:, 2 * LANES :],
        (((1,), (1,)), ((), ())),
        preferred_element_type=jnp.float32,
    ).astype(jnp.bfloat16)


def block(x, weights, s_gate, s_up):
    return pl.pallas_call(
        block_body,
        out_shape=jax.ShapeDtypeStruct(x.shape, jnp.bfloat16),
        compiler_params=ROOM,
    )(x, weights, s_gate, s_up)


def join_body(pieces, before, scale, gain, total, out):
    count = pieces.shape[0]
    added = pieces[0].astype(jnp.float32)
    for j in range(1, count):
        added += pieces[j].astype(jnp.float32)
    values = 0.1 * before[...] + (0.5 / LIFT) * added * scale[...]
    total[...] = values
    meansq = jnp.sum(values * values, axis=1, keepdims=True) / D
    normed = (values * lax.rsqrt(meansq + EPS) * gain[...]).astype(jnp.bfloat16)
    if len(out.shape) == 3:
        for j in range(count):
            out[j] = normed
    else:
        out[...] = normed


def join(pieces, before, scale, gain, copies):
    count, rows, _ = pieces.shape
    shape = (count, rows, D) if copies else (rows, D)
    return pl.pallas_call(
        join_body,
        out_shape=(
            jax.ShapeDtypeStruct((rows, D), jnp.float32),
            jax.ShapeDtypeStruct(shape, jnp.bfloat16),
        ),
        compiler_params=ROOM,
    )(pieces, before, scale[None], gain[None])


def exchange(pieces):
    return lax.all_to_all(pieces, RA, split_axis=0, concat_axis=0, tiled=True)


def copy_for_each(x):
    return exchange(jnp.broadcast_to(x, (lax.axis_size(RA), *x.shape)))


def by_rows(partial_value):
    return exchange(partial_value.reshape(lax.axis_size(RA), -1, D))


def padded(scale):
    return jnp.pad(scale / LIFT, (0, LANES - scale.shape[0]))[None]


def shards(
    tokens,
    gain_first,
    gate_first,
    gate_first_scale,
    up_first,
    up_first_scale,
    down_first,
    down_first_scale,
    gain_second,
    gate_second,
    gate_second_scale,
    up_second,
    up_second_scale,
    down_second,
    down_second_scale,
    gain_last,
):
    count = lax.axis_size(RA)
    packed = pack(gate_first, up_first, down_first, gate_second, up_second, down_second)
    pieces = copy_for_each(tokens)
    weights = lax.all_gather(packed.astype(jnp.float16), CB, axis=0, tiled=True)
    rows = tokens.shape[0] // count
    normed = spread(pieces, gain_first)
    own = lax.dynamic_slice_in_dim(pieces, lax.axis_index(RA) * rows, rows, 1)
    own = jnp.moveaxis(own, 0, 1).reshape(rows, D).astype(jnp.float32)
    w_first, w_second = (w.astype(jnp.bfloat16) for w in jnp.split(weights, 2, axis=1))
    partial_first = block(normed, w_first, padded(gate_first_scale), padded(up_first_scale))
    first, copies = join(by_rows(partial_first), own, down_first_scale, gain_second, True)
    normed = exchange(copies).reshape(-1, D)
    partial_second = block(normed, w_second, padded(gate_second_scale), padded(up_second_scale))
    _, mixed = join(by_rows(partial_second), first, down_second_scale, gain_last, False)
    columns = jnp.moveaxis(mixed.reshape(rows, count, -1), 1, 0)
    return exchange(columns).reshape(tokens.shape)


def solution(mesh):
    torus = Mesh(mesh.devices.reshape(4, 4, 16, 2), ("ra_0", "ra_1", "cb_0", "cb_1"))
    weight, across = P(CB, RA), P(RA, CB)
    return jax.shard_map(
        shards,
        mesh=torus,
        in_specs=(
            P(CB, RA),
            P(),
            weight,
            P(RA),
            weight,
            P(RA),
            across,
            P(),
            P(),
            weight,
            P(RA),
            weight,
            P(RA),
            across,
            P(),
            P(),
        ),
        out_specs=P(CB, RA),
        check_vma=False,
    )
```

```python
import functools

import jax
import jax.numpy as jnp
from jax import lax
from jax.experimental import pallas as pl
from jax.experimental.pallas import tpu as pltpu
from jax.sharding import Mesh
from jax.sharding import PartitionSpec as P


D = 2048
HALF = D // 2
RA = ("ra_0", "ra_1")
CB = ("cb_0", "cb_1")
LANES = 384
TILE = 128
EPS = 1e-06
LIFT = 2.0**18
ROOM = pltpu.CompilerParams(vmem_limit_bytes=20 * 1024 * 1024)
MOST = pltpu.CompilerParams(vmem_limit_bytes=50 * 1024 * 1024)
VMEM = pl.BlockSpec(memory_space=pltpu.VMEM)
HBM = pl.BlockSpec(memory_space=pltpu.HBM)


def pack_body(*refs):
    pieces, (out, held, sems) = refs[:6], refs[6:]
    loads = [pltpu.make_async_copy(p, held.at[j], sems.at[j]) for j, p in enumerate(pieces)]
    for load in loads:
        load.start()
    width = held.shape[2]
    out[...] = jnp.zeros_like(out)
    for j, load in enumerate(loads):
        load.wait()
        out[:, j * LANES : j * LANES + width] = held[j].astype(jnp.bfloat16) * LIFT


def pack(*pieces):
    rows, width = pieces[0].shape
    return pl.pallas_call(
        pack_body,
        in_specs=[HBM] * 6,
        out_shape=jax.ShapeDtypeStruct((rows, 6 * LANES), jnp.bfloat16),
        scratch_shapes=[
            pltpu.VMEM((6, rows, width), jnp.float32),
            pltpu.SemaphoreType.DMA((6,)),
        ],
    )(*pieces)


def halves(left, right):
    low = lax.broadcasted_iota(jnp.int32, left.shape, 1) < TILE // 2
    turn = functools.partial(pltpu.roll, shift=TILE // 2, axis=1)
    return jnp.where(low, left, turn(right)), jnp.where(low, turn(left), right)


def to_split(tiles):
    pairs = [halves(*tiles[j : j + 2]) for j in range(0, len(tiles), 2)]
    return [a for a, _ in pairs] + [b for _, b in pairs]


def from_split(tiles):
    count = len(tiles) // 2
    pairs = [halves(tiles[j], tiles[j + count]) for j in range(count)]
    return [tile for pair in pairs for tile in pair]


def tiles_of(value):
    return [value[:, j : j + TILE] for j in range(0, value.shape[1], TILE)]


def split_row(vector):
    rows = jnp.broadcast_to(vector[...], (8, D))
    return jnp.concatenate(to_split(tiles_of(rows)), axis=1)[:1]


def spread_body(pieces, gain, out, own):
    count, rows, _ = pieces.shape
    total = jnp.zeros((rows, 1), jnp.float32)
    for j in range(count):
        piece = pieces[j].astype(jnp.float32)
        total += jnp.sum(piece * piece, axis=1, keepdims=True)
    scale = lax.rsqrt(total / D + EPS)
    few = own.shape[0]
    start = pl.multiple_of(lax.axis_index(RA) * few, few)
    for j in range(0, count, 2):
        normed, kept = [], []
        for i in (j, j + 1):
            value = pieces[i].astype(jnp.float32)
            normed.append(value * scale * gain[:, i * TILE : (i + 1) * TILE])
            kept.append(pieces[i, pl.ds(start, few), :].astype(jnp.float32))
        for side in (0, 1):
            at = slice(side * HALF + j // 2 * TILE, side * HALF + (j // 2 + 1) * TILE)
            out[:, at] = halves(*normed)[side].astype(jnp.bfloat16)
            own[:, at] = halves(*kept)[side]


def spread(pieces, gain):
    count, rows, _ = pieces.shape
    return pl.pallas_call(
        spread_body,
        out_shape=(
            jax.ShapeDtypeStruct((rows, D), jnp.bfloat16),
            jax.ShapeDtypeStruct((rows // count, D), jnp.float32),
        ),
        compiler_params=ROOM,
    )(pieces, gain[None])


def block_body(x, near, far, s_gate, s_up, out, held, scales, sems):
    loads = [
        [
            pltpu.make_async_copy(
                weights.at[:, pl.ds(j * LANES, LANES)],
                held.at[side, :, pl.ds(j * LANES, LANES)],
                sems.at[side, j],
            )
            for side, weights in enumerate((near, far))
        ]
        for j in range(3)
    ]
    for pair in loads:
        for load in pair:
            load.start()
    scales[...] = jnp.zeros_like(scales)
    scales[0:1, : s_gate.shape[1]] = s_gate[...] / LIFT
    scales[1:2, : s_up.shape[1]] = s_up[...] / LIFT
    core = lax.axis_index("cb_1")
    columns = [
        pl.ds(pl.multiple_of(core * HALF, HALF), HALF),
        pl.ds(pl.multiple_of((1 - core) * HALF, HALF), HALF),
    ]

    def product(j):
        parts = []
        for side in (0, 1):
            loads[j][side].wait()
            part = held[side, :, j * LANES : (j + 1) * LANES]
            parts.append(jnp.dot(x[:, columns[side]], part, preferred_element_type=jnp.float32))
        return (parts[0] + parts[1]) * scales[j : j + 1]

    gate = product(0)
    upper = product(1)
    hidden = (gate / (1.0 + jnp.exp(-gate)) * upper).astype(jnp.bfloat16)
    for side in (0, 1):
        loads[2][side].wait()
        out[:, columns[side]] = lax.dot_general(
            hidden,
            held[side, :, 2 * LANES :],
            (((1,), (1,)), ((), ())),
            preferred_element_type=jnp.float32,
        ).astype(jnp.bfloat16)


def block(x, near, far, s_gate, s_up):
    return pl.pallas_call(
        block_body,
        in_specs=[VMEM, HBM, HBM, VMEM, VMEM],
        out_shape=jax.ShapeDtypeStruct(x.shape, jnp.bfloat16),
        scratch_shapes=[
            pltpu.VMEM((2, *near.shape), jnp.bfloat16),
            pltpu.VMEM((8, LANES), jnp.float32),
            pltpu.SemaphoreType.DMA((2, 3)),
        ],
        compiler_params=MOST,
    )(x, near, far, s_gate[None], s_up[None])


def join_body(last, pieces, before, scale, gain, *outs):
    count = pieces.shape[0]
    added = pieces[0].astype(jnp.float32)
    for j in range(1, count):
        added += pieces[j].astype(jnp.float32)
    values = 0.1 * before[...] + (0.5 / LIFT) * added * split_row(scale)
    meansq = jnp.sum(values * values, axis=1, keepdims=True) / D
    normed = values * lax.rsqrt(meansq + EPS) * split_row(gain)
    if last:
        (out,) = outs
        for j, tile in enumerate(from_split(tiles_of(normed))):
            out[j] = tile.astype(jnp.bfloat16)
    else:
        out, total = outs
        total[...] = values
        for j in range(count):
            out[j] = normed.astype(jnp.bfloat16)


def join(pieces, before, scale, gain, last):
    count, rows, _ = pieces.shape
    shapes = [jax.ShapeDtypeStruct((count, rows, TILE if last else D), jnp.bfloat16)]
    if not last:
        shapes.append(jax.ShapeDtypeStruct((rows, D), jnp.float32))
    return pl.pallas_call(
        functools.partial(join_body, last), out_shape=shapes, compiler_params=ROOM
    )(pieces, before, scale[None], gain[None])


def exchange(pieces):
    return lax.all_to_all(pieces, RA, split_axis=0, concat_axis=0, tiled=True)


def copy_for_each(x):
    return exchange(jnp.broadcast_to(x, (lax.axis_size(RA), *x.shape)))


def by_rows(partial_value):
    return exchange(partial_value.reshape(lax.axis_size(RA), -1, D))


def both_cores(weights):
    near = weights.astype(jnp.bfloat16)
    return near, lax.ppermute(near, "cb_1", ((0, 1), (1, 0)))


def shards(
    tokens,
    gain_first,
    gate_first,
    gate_first_scale,
    up_first,
    up_first_scale,
    down_first,
    down_first_scale,
    gain_second,
    gate_second,
    gate_second_scale,
    up_second,
    up_second_scale,
    down_second,
    down_second_scale,
    gain_last,
):
    packed = pack(gate_first, up_first, down_first.T, gate_second, up_second, down_second.T)
    packed, tokens = lax.optimization_barrier((packed, tokens))
    pieces = copy_for_each(tokens)
    packed = packed.astype(jnp.float16)
    weights = lax.all_gather(packed, "cb_0", axis=0, tiled=True)
    near, far = both_cores(weights[:, : 3 * LANES])
    normed, own = spread(pieces, gain_first)
    partial_first = block(normed, near, far, gate_first_scale, up_first_scale)
    weights, partial_first = lax.optimization_barrier((weights, partial_first))
    near, far = both_cores(weights[:, 3 * LANES :])
    arrived = by_rows(partial_first)
    copies, first = join(arrived, own, down_first_scale, gain_second, False)
    normed = exchange(copies).reshape(-1, D)
    partial_second = block(normed, near, far, gate_second_scale, up_second_scale)
    (columns,) = join(by_rows(partial_second), first, down_second_scale, gain_last, True)
    return exchange(columns).reshape(tokens.shape)


def solution(mesh):
    torus = Mesh(mesh.devices.reshape(4, 4, 16, 2), ("ra_0", "ra_1", "cb_0", "cb_1"))
    weight, across = P(CB, RA), P(RA, CB)
    return jax.shard_map(
        shards,
        mesh=torus,
        in_specs=(
            P(CB, RA),
            P(),
            weight,
            P(RA),
            weight,
            P(RA),
            across,
            P(),
            P(),
            weight,
            P(RA),
            weight,
            P(RA),
            across,
            P(),
            P(),
        ),
        out_specs=P(CB, RA),
        check_vma=False,
    )
```

```python
import functools

import jax
import jax.numpy as jnp
from jax import lax
from jax.experimental import pallas as pl
from jax.experimental.pallas import tpu as pltpu
from jax.sharding import Mesh
from jax.sharding import PartitionSpec as P


D = 2048
HALF = D // 2
RA = ("ra_0", "ra_1")
CB = ("cb_0", "cb_1")
TILE = 128
TILES = 17
PART = 9
WIDE = 4 * TILE
EPS = 1e-06
LIFT = 2.0**18
ROOM = pltpu.CompilerParams(vmem_limit_bytes=20 * 1024 * 1024)
MORE = pltpu.CompilerParams(vmem_limit_bytes=44 * 1024 * 1024)
MOST = pltpu.CompilerParams(vmem_limit_bytes=50 * 1024 * 1024)
VMEM = pl.BlockSpec(memory_space=pltpu.VMEM)
HBM = pl.BlockSpec(memory_space=pltpu.HBM)


def pack_body(*refs):
    pieces, tokens, out, copies, held, wide, own, sems, copy_sems = refs[:6], *refs[6:]
    loads = [pltpu.make_async_copy(p, held.at[j], sems.at[j]) for j, p in enumerate(pieces)]
    token_load = pltpu.make_async_copy(tokens, own, sems.at[len(pieces)])
    sends = [
        pltpu.make_async_copy(own, copies.at[j], copy_sems.at[j]) for j in range(copies.shape[0])
    ]
    token_load.start()
    for load in loads:
        load.start()
    token_load.wait()
    for send in sends:
        send.start()
    rows, width = held.shape[1:]
    wide[...] = jnp.zeros_like(wide)
    tiles = [None] * TILES
    for j, load in enumerate(loads):
        load.wait()
        wide[:, :width] = held[j]
        first, shift = divmod(j * width, TILE)
        turned = pltpu.roll(wide[...], shift, axis=1) if shift else wide[...]
        for k in range(-(-(width + shift) // TILE)):
            part = turned[:, k * TILE : (k + 1) * TILE]
            old = tiles[first + k]
            tiles[first + k] = part if old is None else old + part
    for j, tile in enumerate(tiles):
        out[j * rows : (j + 1) * rows] = tile.astype(jnp.bfloat16) * LIFT
    for send in sends:
        send.wait()


def pack(tokens, *pieces):
    rows, width = pieces[0].shape
    count = lax.axis_size(RA)
    return pl.pallas_call(
        pack_body,
        in_specs=[HBM] * 7,
        out_specs=[VMEM, HBM],
        out_shape=(
            jax.ShapeDtypeStruct((TILES * rows, TILE), jnp.bfloat16),
            jax.ShapeDtypeStruct((count, *tokens.shape), tokens.dtype),
        ),
        scratch_shapes=[
            pltpu.VMEM((6, rows, width), jnp.float32),
            pltpu.VMEM((rows, WIDE), jnp.float32),
            pltpu.VMEM(tokens.shape, tokens.dtype),
            pltpu.SemaphoreType.DMA((7,)),
            pltpu.SemaphoreType.DMA((count,)),
        ],
    )(*pieces, tokens)


def halves(left, right):
    low = lax.broadcasted_iota(jnp.int32, left.shape, 1) < TILE // 2
    turn = functools.partial(pltpu.roll, shift=TILE // 2, axis=1)
    return jnp.where(low, left, turn(right)), jnp.where(low, turn(left), right)


def to_split(tiles):
    pairs = [halves(*tiles[j : j + 2]) for j in range(0, len(tiles), 2)]
    return [a for a, _ in pairs] + [b for _, b in pairs]


def from_split(tiles):
    count = len(tiles) // 2
    pairs = [halves(tiles[j], tiles[j + count]) for j in range(count)]
    return [tile for pair in pairs for tile in pair]


def tiles_of(value):
    return [value[:, j : j + TILE] for j in range(0, value.shape[1], TILE)]


def split_row(vector):
    rows = jnp.broadcast_to(vector[...], (8, D))
    return jnp.concatenate(to_split(tiles_of(rows)), axis=1)[:1]


def spread_body(pieces, gain, out, own):
    count, rows, _ = pieces.shape
    total = jnp.zeros((rows, 1), jnp.float32)
    for j in range(count):
        piece = pieces[j].astype(jnp.float32)
        total += jnp.sum(piece * piece, axis=1, keepdims=True)
    scale = lax.rsqrt(total / D + EPS)
    few = own.shape[0]
    start = pl.multiple_of(lax.axis_index(RA) * few, few)
    for j in range(0, count, 2):
        normed, kept = [], []
        for i in (j, j + 1):
            value = pieces[i].astype(jnp.float32)
            normed.append(value * scale * gain[:, i * TILE : (i + 1) * TILE])
            kept.append(pieces[i, pl.ds(start, few), :].astype(jnp.float32))
        for side in (0, 1):
            at = slice(side * HALF + j // 2 * TILE, side * HALF + (j // 2 + 1) * TILE)
            out[:, at] = halves(*normed)[side].astype(jnp.bfloat16)
            own[:, at] = halves(*kept)[side]


def spread(pieces, gain):
    count, rows, _ = pieces.shape
    return pl.pallas_call(
        spread_body,
        out_shape=(
            jax.ShapeDtypeStruct((rows, D), jnp.bfloat16),
            jax.ShapeDtypeStruct((rows // count, D), jnp.float32),
        ),
        compiler_params=ROOM,
    )(pieces, gain[None])


def tile_loads(weights, held, sems):
    rows = held.shape[1]
    return [
        pltpu.make_async_copy(
            weights.at[:, pl.ds(j * rows, rows)], held.at[:, :, pl.ds(j * TILE, TILE)], sems.at[j]
        )
        for j in range(PART)
    ]


def stage_body(weights, out, sems):
    loads = tile_loads(weights, out, sems)
    for load in loads:
        load.start()
    for load in loads:
        load.wait()


def stage(weights):
    groups, rows = weights.shape[0], weights.shape[1] // PART
    return pl.pallas_call(
        stage_body,
        in_specs=[HBM],
        out_shape=jax.ShapeDtypeStruct((groups, rows, PART * TILE), jnp.bfloat16),
        scratch_shapes=[pltpu.SemaphoreType.DMA((PART,))],
        compiler_params=ROOM,
    )(weights)


def block_body(start, x, near, far, s_gate, s_up, out, scales, *scratch):
    if scratch:
        held, sems = scratch
        loads = tile_loads(far, held, sems)
        for load in loads:
            load.start()
    else:
        held, loads = far, []
    width = s_gate.shape[1]
    scales[...] = jnp.zeros_like(scales)
    scales[0:1, :width] = s_gate[...] / LIFT
    scales[1:2, :width] = s_up[...] / LIFT
    down = (start + 2 * width) // TILE * TILE
    place = start + 2 * width - down
    placed = pltpu.roll(scales[...], place, axis=1)
    core = lax.axis_index("cb_1")
    columns = [
        pl.ds(pl.multiple_of(core * HALF, HALF), HALF),
        pl.ds(pl.multiple_of((1 - core) * HALF, HALF), HALF),
    ]
    across = -(-(start + 2 * width) // TILE)

    def product(side, weights):
        part = weights[:, :, : across * TILE].reshape(HALF, across * TILE)
        return jnp.dot(x[:, columns[side]], part, preferred_element_type=jnp.float32)

    both = product(0, near)
    for load in loads[:across]:
        load.wait()
    both += product(1, held)

    def turned(at):
        return pltpu.roll(both, (place - at) % both.shape[1], axis=1)[:, :WIDE]

    gate = turned(start) * placed[0:1]
    upper = turned(start + width) * placed[1:2]
    hidden = (gate / (1.0 + jnp.exp(-gate)) * upper).astype(jnp.bfloat16)
    for load in loads[across:]:
        load.wait()
    for side, weights in enumerate((near, held)):
        out[:, columns[side]] = lax.dot_general(
            hidden,
            weights[:, :, down : down + WIDE].reshape(HALF, WIDE),
            (((1,), (1,)), ((), ())),
            preferred_element_type=jnp.float32,
        ).astype(jnp.bfloat16)


def block(x, near, far, start, s_gate, s_up):
    scratch = [pltpu.VMEM((8, WIDE), jnp.float32)]
    loaded = far.shape == near.shape
    if not loaded:
        scratch += [pltpu.VMEM(near.shape, jnp.bfloat16), pltpu.SemaphoreType.DMA((PART,))]
    return pl.pallas_call(
        functools.partial(block_body, start),
        in_specs=[VMEM, VMEM, VMEM if loaded else HBM, VMEM, VMEM],
        out_shape=jax.ShapeDtypeStruct(x.shape, jnp.bfloat16),
        scratch_shapes=scratch,
        compiler_params=MORE,
    )(x, near, far, s_gate[None], s_up[None])


def join_body(last, pieces, before, scale, gain, *outs):
    count = pieces.shape[0]
    added = pieces[0].astype(jnp.float32)
    for j in range(1, count):
        added += pieces[j].astype(jnp.float32)
    values = 0.1 * before[...] + (0.5 / LIFT) * added * split_row(scale)
    meansq = jnp.sum(values * values, axis=1, keepdims=True) / D
    normed = values * lax.rsqrt(meansq + EPS) * split_row(gain)
    if last:
        (out,) = outs
        for j, tile in enumerate(from_split(tiles_of(normed))):
            out[j] = tile.astype(jnp.bfloat16)
    else:
        out, total = outs
        total[...] = values
        for j in range(count):
            out[j] = normed.astype(jnp.bfloat16)


def join(pieces, before, scale, gain, last):
    count, rows, _ = pieces.shape
    shapes = [jax.ShapeDtypeStruct((count, rows, TILE if last else D), jnp.bfloat16)]
    if not last:
        shapes.append(jax.ShapeDtypeStruct((rows, D), jnp.float32))
    return pl.pallas_call(
        functools.partial(join_body, last), out_shape=shapes, compiler_params=MOST
    )(pieces, before, scale[None], gain[None])


def exchange(pieces):
    return lax.all_to_all(pieces, RA, split_axis=0, concat_axis=0, tiled=True)


def by_rows(partial_value):
    return exchange(partial_value.reshape(lax.axis_size(RA), -1, D))


def both_cores(weights):
    near = weights.astype(jnp.bfloat16)
    return near, lax.ppermute(near, "cb_1", ((0, 1), (1, 0)))


def shards(
    tokens,
    gain_first,
    gate_first,
    gate_first_scale,
    up_first,
    up_first_scale,
    down_first,
    down_first_scale,
    gain_second,
    gate_second,
    gate_second_scale,
    up_second,
    up_second_scale,
    down_second,
    down_second_scale,
    gain_last,
):
    packed, copies = pack(
        tokens, gate_first, up_first, down_first.T, gate_second, up_second, down_second.T
    )
    pieces = exchange(copies)
    packed = lax.optimization_barrier(packed.astype(jnp.float16))
    gathered = lax.all_gather(packed.reshape(-1), "cb_0", axis=0, tiled=True)
    rows, width = gate_first.shape
    weights = gathered.reshape(-1, TILES * rows, TILE)
    later, start = divmod(3 * width, TILE)
    near, far = both_cores(weights[:, : PART * rows])
    near = stage(near)
    normed, own = spread(pieces, gain_first)
    partial_first = block(normed, near, far, 0, gate_first_scale, up_first_scale)
    weights, partial_first = lax.optimization_barrier((weights, partial_first))
    near, far = both_cores(weights[:, later * rows :])
    arrived = by_rows(partial_first)
    copies, first = join(arrived, own, down_first_scale, gain_second, False)
    normed = exchange(copies).reshape(-1, D)
    near, far = stage(near), stage(far)
    partial_second = block(normed, near, far, start, gate_second_scale, up_second_scale)
    (columns,) = join(by_rows(partial_second), first, down_second_scale, gain_last, True)
    return exchange(columns).reshape(tokens.shape)


def solution(mesh):
    torus = Mesh(mesh.devices.reshape(4, 4, 16, 2), ("ra_0", "ra_1", "cb_0", "cb_1"))
    weight, across = P(CB, RA), P(RA, CB)
    return jax.shard_map(
        shards,
        mesh=torus,
        in_specs=(
            P(CB, RA),
            P(),
            weight,
            P(RA),
            weight,
            P(RA),
            across,
            P(),
            P(),
            weight,
            P(RA),
            weight,
            P(RA),
            across,
            P(),
            P(),
        ),
        out_specs=P(CB, RA),
        check_vma=False,
    )
```

```python
import functools

import jax
import jax.numpy as jnp
from jax import lax
from jax.experimental import pallas as pl
from jax.experimental.pallas import tpu as pltpu
from jax.sharding import Mesh
from jax.sharding import PartitionSpec as P


D = 2048
HALF = D // 2
RA = ("ra_0", "ra_1")
CB = ("cb_0", "cb_1")
TILE = 128
TILES = 17
PART = 9
WIDE = 4 * TILE
EPS = 1e-06
LIFT = 2.0**18
ROOM = pltpu.CompilerParams(vmem_limit_bytes=20 * 1024 * 1024)
MOST = pltpu.CompilerParams(vmem_limit_bytes=24 * 1024 * 1024)
VMEM = pl.BlockSpec(memory_space=pltpu.VMEM)
HBM = pl.BlockSpec(memory_space=pltpu.HBM)


def pack_body(*refs):
    pieces, tokens, out, copies, held, wide, own, sems, copy_sems = refs[:6], *refs[6:]
    loads = [pltpu.make_async_copy(p, held.at[j], sems.at[j]) for j, p in enumerate(pieces)]
    token_load = pltpu.make_async_copy(tokens, own, sems.at[len(pieces)])
    sends = [
        pltpu.make_async_copy(own, copies.at[j], copy_sems.at[j]) for j in range(copies.shape[0])
    ]
    token_load.start()
    for load in loads:
        load.start()
    token_load.wait()
    for send in sends:
        send.start()
    rows, width = held.shape[1:]
    wide[...] = jnp.zeros_like(wide)
    tiles = [None] * TILES
    for j, load in enumerate(loads):
        load.wait()
        wide[:, :width] = held[j]
        first, shift = divmod(j * width, TILE)
        turned = pltpu.roll(wide[...], shift, axis=1) if shift else wide[...]
        for k in range(-(-(width + shift) // TILE)):
            part = turned[:, k * TILE : (k + 1) * TILE]
            old = tiles[first + k]
            tiles[first + k] = part if old is None else old + part
    for j, tile in enumerate(tiles):
        out[j * rows : (j + 1) * rows] = tile.astype(jnp.bfloat16) * LIFT
    for send in sends:
        send.wait()


def pack(tokens, *pieces):
    rows, width = pieces[0].shape
    count = lax.axis_size(RA)
    return pl.pallas_call(
        pack_body,
        in_specs=[HBM] * 7,
        out_specs=[VMEM, HBM],
        out_shape=(
            jax.ShapeDtypeStruct((TILES * rows, TILE), jnp.bfloat16),
            jax.ShapeDtypeStruct((count, *tokens.shape), tokens.dtype),
        ),
        scratch_shapes=[
            pltpu.VMEM((6, rows, width), jnp.float32),
            pltpu.VMEM((rows, WIDE), jnp.float32),
            pltpu.VMEM(tokens.shape, tokens.dtype),
            pltpu.SemaphoreType.DMA((7,)),
            pltpu.SemaphoreType.DMA((count,)),
        ],
    )(*pieces, tokens)


def halves(left, right):
    low = lax.broadcasted_iota(jnp.int32, left.shape, 1) < TILE // 2
    turn = functools.partial(pltpu.roll, shift=TILE // 2, axis=1)
    return jnp.where(low, left, turn(right)), jnp.where(low, turn(left), right)


def to_split(tiles):
    pairs = [halves(*tiles[j : j + 2]) for j in range(0, len(tiles), 2)]
    return [a for a, _ in pairs] + [b for _, b in pairs]


def from_split(tiles):
    count = len(tiles) // 2
    pairs = [halves(tiles[j], tiles[j + count]) for j in range(count)]
    return [tile for pair in pairs for tile in pair]


def tiles_of(value):
    return [value[:, j : j + TILE] for j in range(0, value.shape[1], TILE)]


def split_row(vector):
    rows = jnp.broadcast_to(vector[...], (8, D))
    return jnp.concatenate(to_split(tiles_of(rows)), axis=1)[:1]


def spread_body(pieces, gain, out, own):
    count, rows, _ = pieces.shape
    total = jnp.zeros((rows, 1), jnp.float32)
    for j in range(count):
        piece = pieces[j].astype(jnp.float32)
        total += jnp.sum(piece * piece, axis=1, keepdims=True)
    scale = lax.rsqrt(total / D + EPS)
    few = own.shape[0]
    start = pl.multiple_of(lax.axis_index(RA) * few, few)
    for j in range(0, count, 2):
        normed, kept = [], []
        for i in (j, j + 1):
            value = pieces[i].astype(jnp.float32)
            normed.append(value * scale * gain[:, i * TILE : (i + 1) * TILE])
            kept.append(pieces[i, pl.ds(start, few), :].astype(jnp.float32))
        for side in (0, 1):
            at = slice(side * HALF + j // 2 * TILE, side * HALF + (j // 2 + 1) * TILE)
            out[:, at] = halves(*normed)[side].astype(jnp.bfloat16)
            own[:, at] = halves(*kept)[side]


def spread(pieces, gain):
    count, rows, _ = pieces.shape
    return pl.pallas_call(
        spread_body,
        out_shape=(
            jax.ShapeDtypeStruct((rows, D), jnp.bfloat16),
            jax.ShapeDtypeStruct((rows // count, D), jnp.float32),
        ),
        compiler_params=ROOM,
    )(pieces, gain[None])


def block_body(start, x, near, far, s_gate, s_up, out, held, scales, sems):
    rows = near.shape[1] // PART
    loads = [
        [
            pltpu.make_async_copy(
                weights.at[:, pl.ds(j * rows, rows)],
                held.at[side, :, :, pl.ds(j * TILE, TILE)],
                sems.at[side, j],
            )
            for side, weights in enumerate((near, far))
        ]
        for j in range(PART)
    ]
    for pair in loads:
        for load in pair:
            load.start()
    width = s_gate.shape[1]
    scales[...] = jnp.zeros_like(scales)
    scales[0:1, :width] = s_gate[...] / LIFT
    scales[1:2, :width] = s_up[...] / LIFT
    down = (start + 2 * width) // TILE * TILE
    place = start + 2 * width - down
    placed = pltpu.roll(scales[...], place, axis=1)
    core = lax.axis_index("cb_1")
    columns = [
        pl.ds(pl.multiple_of(core * HALF, HALF), HALF),
        pl.ds(pl.multiple_of((1 - core) * HALF, HALF), HALF),
    ]
    across = -(-(start + 2 * width) // TILE)
    both = jnp.zeros((x.shape[0], across * TILE), jnp.float32)
    for side in (0, 1):
        for j in range(across):
            loads[j][side].wait()
        part = held[side, :, :, : across * TILE].reshape(HALF, across * TILE)
        both += jnp.dot(x[:, columns[side]], part, preferred_element_type=jnp.float32)

    def turned(at):
        return pltpu.roll(both, (place - at) % both.shape[1], axis=1)[:, :WIDE]

    gate = turned(start) * placed[0:1]
    upper = turned(start + width) * placed[1:2]
    hidden = (gate / (1.0 + jnp.exp(-gate)) * upper).astype(jnp.bfloat16)
    for side in (0, 1):
        for j in range(across, PART):
            loads[j][side].wait()
        out[:, columns[side]] = lax.dot_general(
            hidden,
            held[side, :, :, down : down + WIDE].reshape(HALF, WIDE),
            (((1,), (1,)), ((), ())),
            preferred_element_type=jnp.float32,
        ).astype(jnp.bfloat16)


def block(x, near, far, start, s_gate, s_up):
    groups, rows = near.shape[0], near.shape[1] // PART
    return pl.pallas_call(
        functools.partial(block_body, start),
        in_specs=[VMEM, HBM, HBM, VMEM, VMEM],
        out_shape=jax.ShapeDtypeStruct(x.shape, jnp.bfloat16),
        scratch_shapes=[
            pltpu.VMEM((2, groups, rows, PART * TILE), jnp.bfloat16),
            pltpu.VMEM((8, WIDE), jnp.float32),
            pltpu.SemaphoreType.DMA((2, PART)),
        ],
        compiler_params=MOST,
    )(x, near, far, s_gate[None], s_up[None])


def join_body(last, pieces, before, scale, gain, *outs):
    count = pieces.shape[0]
    added = pieces[0].astype(jnp.float32)
    for j in range(1, count):
        added += pieces[j].astype(jnp.float32)
    values = 0.1 * before[...] + (0.5 / LIFT) * added * split_row(scale)
    meansq = jnp.sum(values * values, axis=1, keepdims=True) / D
    normed = values * lax.rsqrt(meansq + EPS) * split_row(gain)
    if last:
        (out,) = outs
        for j, tile in enumerate(from_split(tiles_of(normed))):
            out[j] = tile.astype(jnp.bfloat16)
    else:
        out, total = outs
        total[...] = values
        for j in range(count):
            out[j] = normed.astype(jnp.bfloat16)


def join(pieces, before, scale, gain, last):
    count, rows, _ = pieces.shape
    shapes = [jax.ShapeDtypeStruct((count, rows, TILE if last else D), jnp.bfloat16)]
    if not last:
        shapes.append(jax.ShapeDtypeStruct((rows, D), jnp.float32))
    return pl.pallas_call(
        functools.partial(join_body, last), out_shape=shapes, compiler_params=ROOM
    )(pieces, before, scale[None], gain[None])


def exchange(pieces):
    return lax.all_to_all(pieces, RA, split_axis=0, concat_axis=0, tiled=True)


def by_rows(partial_value):
    return exchange(partial_value.reshape(lax.axis_size(RA), -1, D))


def both_cores(weights):
    near = weights.astype(jnp.bfloat16)
    return near, lax.ppermute(near, "cb_1", ((0, 1), (1, 0)))


def shards(
    tokens,
    gain_first,
    gate_first,
    gate_first_scale,
    up_first,
    up_first_scale,
    down_first,
    down_first_scale,
    gain_second,
    gate_second,
    gate_second_scale,
    up_second,
    up_second_scale,
    down_second,
    down_second_scale,
    gain_last,
):
    packed, copies = pack(
        tokens, gate_first, up_first, down_first.T, gate_second, up_second, down_second.T
    )
    pieces = exchange(copies)
    packed = packed.reshape(-1).astype(jnp.float16)
    gathered = lax.all_gather(packed, "cb_0", axis=0, tiled=True)
    rows, width = gate_first.shape
    weights = gathered.reshape(-1, TILES * rows, TILE)
    later, start = divmod(3 * width, TILE)
    near, far = both_cores(weights[:, : PART * rows])
    normed, own = spread(pieces, gain_first)
    partial_first = block(normed, near, far, 0, gate_first_scale, up_first_scale)
    weights, partial_first = lax.optimization_barrier((weights, partial_first))
    near, far = both_cores(weights[:, later * rows :])
    arrived = by_rows(partial_first)
    copies, first = join(arrived, own, down_first_scale, gain_second, False)
    normed = exchange(copies).reshape(-1, D)
    partial_second = block(normed, near, far, start, gate_second_scale, up_second_scale)
    (columns,) = join(by_rows(partial_second), first, down_second_scale, gain_last, True)
    return exchange(columns).reshape(tokens.shape)


def solution(mesh):
    torus = Mesh(mesh.devices.reshape(4, 4, 16, 2), ("ra_0", "ra_1", "cb_0", "cb_1"))
    weight, across = P(CB, RA), P(RA, CB)
    return jax.shard_map(
        shards,
        mesh=torus,
        in_specs=(
            P(CB, RA),
            P(),
            weight,
            P(RA),
            weight,
            P(RA),
            across,
            P(),
            P(),
            weight,
            P(RA),
            weight,
            P(RA),
            across,
            P(),
            P(),
        ),
        out_specs=P(CB, RA),
        check_vma=False,
    )
```

```python
import functools

import jax
import jax.numpy as jnp
from jax import lax
from jax.experimental import pallas as pl
from jax.experimental.pallas import tpu as pltpu
from jax.sharding import Mesh
from jax.sharding import PartitionSpec as P


D = 2048
HALF = D // 2
RA = ("ra_0", "ra_1")
CB = ("cb_0", "cb_1")
TILE = 128
TILES = 17
PART = 9
WIDE = 4 * TILE
EPS = 1e-06
LIFT = 2.0**18
ROOM = pltpu.CompilerParams(vmem_limit_bytes=20 * 1024 * 1024)
MOST = pltpu.CompilerParams(vmem_limit_bytes=24 * 1024 * 1024)
VMEM = pl.BlockSpec(memory_space=pltpu.VMEM)
HBM = pl.BlockSpec(memory_space=pltpu.HBM)


def pack_body(*refs):
    pieces, tokens, out, copies, held, wide, own, sems, copy_sems = refs[:6], *refs[6:]
    loads = [pltpu.make_async_copy(p, held.at[j], sems.at[j]) for j, p in enumerate(pieces)]
    token_load = pltpu.make_async_copy(tokens, own, sems.at[len(pieces)])
    sends = [
        pltpu.make_async_copy(own, copies.at[j], copy_sems.at[j]) for j in range(copies.shape[0])
    ]
    token_load.start()
    for load in loads:
        load.start()
    token_load.wait()
    for send in sends:
        send.start()
    rows, width = held.shape[1:]
    wide[...] = jnp.zeros_like(wide)
    tiles = [None] * TILES
    for j, load in enumerate(loads):
        load.wait()
        wide[:, :width] = held[j]
        first, shift = divmod(j * width, TILE)
        turned = pltpu.roll(wide[...], shift, axis=1) if shift else wide[...]
        for k in range(-(-(width + shift) // TILE)):
            part = turned[:, k * TILE : (k + 1) * TILE]
            old = tiles[first + k]
            tiles[first + k] = part if old is None else old + part
    for j, tile in enumerate(tiles):
        out[j * rows : (j + 1) * rows] = tile.astype(jnp.bfloat16) * LIFT
    for send in sends:
        send.wait()


def pack(tokens, *pieces):
    rows, width = pieces[0].shape
    count = lax.axis_size(RA)
    return pl.pallas_call(
        pack_body,
        in_specs=[HBM] * 7,
        out_specs=[VMEM, HBM],
        out_shape=(
            jax.ShapeDtypeStruct((TILES * rows, TILE), jnp.bfloat16),
            jax.ShapeDtypeStruct((count, *tokens.shape), tokens.dtype),
        ),
        scratch_shapes=[
            pltpu.VMEM((6, rows, width), jnp.float32),
            pltpu.VMEM((rows, WIDE), jnp.float32),
            pltpu.VMEM(tokens.shape, tokens.dtype),
            pltpu.SemaphoreType.DMA((7,)),
            pltpu.SemaphoreType.DMA((count,)),
        ],
    )(*pieces, tokens)


def halves(left, right):
    low = lax.broadcasted_iota(jnp.int32, left.shape, 1) < TILE // 2
    turn = functools.partial(pltpu.roll, shift=TILE // 2, axis=1)
    return jnp.where(low, left, turn(right)), jnp.where(low, turn(left), right)


def to_split(tiles):
    pairs = [halves(*tiles[j : j + 2]) for j in range(0, len(tiles), 2)]
    return [a for a, _ in pairs] + [b for _, b in pairs]


def from_split(tiles):
    count = len(tiles) // 2
    pairs = [halves(tiles[j], tiles[j + count]) for j in range(count)]
    return [tile for pair in pairs for tile in pair]


def tiles_of(value):
    return [value[:, j : j + TILE] for j in range(0, value.shape[1], TILE)]


def split_row(vector):
    rows = jnp.broadcast_to(vector[...], (8, D))
    return jnp.concatenate(to_split(tiles_of(rows)), axis=1)[:1]


def spread_body(pieces, gain, out, own):
    count, rows, _ = pieces.shape
    total = jnp.zeros((rows, 1), jnp.float32)
    for j in range(count):
        piece = pieces[j].astype(jnp.float32)
        total += jnp.sum(piece * piece, axis=1, keepdims=True)
    scale = lax.rsqrt(total / D + EPS)
    few = own.shape[0]
    start = pl.multiple_of(lax.axis_index(RA) * few, few)
    for j in range(0, count, 2):
        normed, kept = [], []
        for i in (j, j + 1):
            value = pieces[i].astype(jnp.float32)
            normed.append(value * scale * gain[:, i * TILE : (i + 1) * TILE])
            kept.append(pieces[i, pl.ds(start, few), :].astype(jnp.float32))
        for side in (0, 1):
            at = slice(side * HALF + j // 2 * TILE, side * HALF + (j // 2 + 1) * TILE)
            out[:, at] = halves(*normed)[side].astype(jnp.bfloat16)
            own[:, at] = halves(*kept)[side]


def spread(pieces, gain):
    count, rows, _ = pieces.shape
    return pl.pallas_call(
        spread_body,
        out_shape=(
            jax.ShapeDtypeStruct((rows, D), jnp.bfloat16),
            jax.ShapeDtypeStruct((rows // count, D), jnp.float32),
        ),
        compiler_params=ROOM,
    )(pieces, gain[None])


def side_by_side(weights, first, last):
    groups, total, _ = weights.shape
    rows = total // PART
    tiles = [
        weights[:, j * rows : (j + 1) * rows, :].reshape(groups * rows, TILE)
        for j in range(first, last)
    ]
    return jnp.concatenate(tiles, axis=1)


def block_body(start, x, near, far, s_gate, s_up, out, held, scales, sems):
    pieces = sems.shape[0]
    groups = held.shape[0] // pieces
    loads = [
        pltpu.make_async_copy(
            far.at[pl.ds(j * groups, groups)], held.at[pl.ds(j * groups, groups)], sems.at[j]
        )
        for j in range(pieces)
    ]
    for load in loads:
        load.start()
    width = s_gate.shape[1]
    scales[...] = jnp.zeros_like(scales)
    scales[0:1, :width] = s_gate[...] / LIFT
    scales[1:2, :width] = s_up[...] / LIFT
    down = (start + 2 * width) // TILE
    place = start + 2 * width - down * TILE
    placed = pltpu.roll(scales[...], place, axis=1)
    core = lax.axis_index("cb_1")
    columns = [
        pl.ds(pl.multiple_of(core * HALF, HALF), HALF),
        pl.ds(pl.multiple_of((1 - core) * HALF, HALF), HALF),
    ]
    across = -(-(start + 2 * width) // TILE)

    def product(side, weights):
        part = side_by_side(weights, 0, across)
        return jnp.dot(x[:, columns[side]], part, preferred_element_type=jnp.float32)

    both = product(0, near)
    for load in loads:
        load.wait()
    both += product(1, held)

    def turned(at):
        return pltpu.roll(both, (place - at) % both.shape[1], axis=1)[:, :WIDE]

    gate = turned(start) * placed[0:1]
    upper = turned(start + width) * placed[1:2]
    hidden = (gate / (1.0 + jnp.exp(-gate)) * upper).astype(jnp.bfloat16)
    for side, weights in enumerate((near, held)):
        out[:, columns[side]] = lax.dot_general(
            hidden,
            side_by_side(weights, down, down + WIDE // TILE),
            (((1,), (1,)), ((), ())),
            preferred_element_type=jnp.float32,
        ).astype(jnp.bfloat16)


def block(x, near, far, start, s_gate, s_up):
    return pl.pallas_call(
        functools.partial(block_body, start),
        in_specs=[VMEM, VMEM, HBM, VMEM, VMEM],
        out_shape=jax.ShapeDtypeStruct(x.shape, jnp.bfloat16),
        scratch_shapes=[
            pltpu.VMEM(far.shape, jnp.bfloat16),
            pltpu.VMEM((8, WIDE), jnp.float32),
            pltpu.SemaphoreType.DMA((4,)),
        ],
        compiler_params=MOST,
    )(x, near, far, s_gate[None], s_up[None])


def join_body(last, pieces, before, scale, gain, *outs):
    count = pieces.shape[0]
    added = pieces[0].astype(jnp.float32)
    for j in range(1, count):
        added += pieces[j].astype(jnp.float32)
    values = 0.1 * before[...] + (0.5 / LIFT) * added * split_row(scale)
    meansq = jnp.sum(values * values, axis=1, keepdims=True) / D
    normed = values * lax.rsqrt(meansq + EPS) * split_row(gain)
    if last:
        (out,) = outs
        for j, tile in enumerate(from_split(tiles_of(normed))):
            out[j] = tile.astype(jnp.bfloat16)
    else:
        out, total = outs
        total[...] = values
        for j in range(count):
            out[j] = normed.astype(jnp.bfloat16)


def join(pieces, before, scale, gain, last):
    count, rows, _ = pieces.shape
    shapes = [jax.ShapeDtypeStruct((count, rows, TILE if last else D), jnp.bfloat16)]
    if not last:
        shapes.append(jax.ShapeDtypeStruct((rows, D), jnp.float32))
    return pl.pallas_call(
        functools.partial(join_body, last), out_shape=shapes, compiler_params=ROOM
    )(pieces, before, scale[None], gain[None])


def exchange(pieces):
    return lax.all_to_all(pieces, RA, split_axis=0, concat_axis=0, tiled=True)


def by_rows(partial_value):
    return exchange(partial_value.reshape(lax.axis_size(RA), -1, D))


def both_cores(weights):
    near = weights.astype(jnp.bfloat16)
    return near, lax.ppermute(near, "cb_1", ((0, 1), (1, 0)))


def shards(
    tokens,
    gain_first,
    gate_first,
    gate_first_scale,
    up_first,
    up_first_scale,
    down_first,
    down_first_scale,
    gain_second,
    gate_second,
    gate_second_scale,
    up_second,
    up_second_scale,
    down_second,
    down_second_scale,
    gain_last,
):
    packed, copies = pack(
        tokens, gate_first, up_first, down_first.T, gate_second, up_second, down_second.T
    )
    pieces = exchange(copies)
    packed = packed.reshape(-1).astype(jnp.float16)
    gathered = lax.all_gather(packed, "cb_0", axis=0, tiled=True)
    rows, width = gate_first.shape
    weights = gathered.reshape(-1, TILES * rows, TILE)
    later, start = divmod(3 * width, TILE)
    near, far = both_cores(weights[:, : PART * rows])
    normed, own = spread(pieces, gain_first)
    partial_first = block(normed, near, far, 0, gate_first_scale, up_first_scale)
    weights, partial_first = lax.optimization_barrier((weights, partial_first))
    near, far = both_cores(weights[:, later * rows :])
    arrived = by_rows(partial_first)
    copies, first = join(arrived, own, down_first_scale, gain_second, False)
    normed = exchange(copies).reshape(-1, D)
    partial_second = block(normed, near, far, start, gate_second_scale, up_second_scale)
    (columns,) = join(by_rows(partial_second), first, down_second_scale, gain_last, True)
    return exchange(columns).reshape(tokens.shape)


def solution(mesh):
    torus = Mesh(mesh.devices.reshape(4, 4, 16, 2), ("ra_0", "ra_1", "cb_0", "cb_1"))
    weight, across = P(CB, RA), P(RA, CB)
    return jax.shard_map(
        shards,
        mesh=torus,
        in_specs=(
            P(CB, RA),
            P(),
            weight,
            P(RA),
            weight,
            P(RA),
            across,
            P(),
            P(),
            weight,
            P(RA),
            weight,
            P(RA),
            across,
            P(),
            P(),
        ),
        out_specs=P(CB, RA),
        check_vma=False,
    )
```

```python
import functools

import jax
import jax.numpy as jnp
from jax import lax
from jax.experimental import pallas as pl
from jax.experimental.pallas import tpu as pltpu
from jax.sharding import Mesh
from jax.sharding import PartitionSpec as P


D = 2048
HALF = D // 2
RA = ("ra_0", "ra_1")
CB = ("cb_0", "cb_1")
TILE = 128
TILES = 17
PART = 9
WIDE = 4 * TILE
EPS = 1e-06
LIFT = 2.0**18
ROOM = pltpu.CompilerParams(vmem_limit_bytes=20 * 1024 * 1024)
VMEM = pl.BlockSpec(memory_space=pltpu.VMEM)
HBM = pl.BlockSpec(memory_space=pltpu.HBM)


def pack_body(*refs):
    pieces, tokens, out, copies, held, wide, own, sems, copy_sems = refs[:6], *refs[6:]
    loads = [pltpu.make_async_copy(p, held.at[j], sems.at[j]) for j, p in enumerate(pieces)]
    token_load = pltpu.make_async_copy(tokens, own, sems.at[len(pieces)])
    sends = [
        pltpu.make_async_copy(own, copies.at[j], copy_sems.at[j]) for j in range(copies.shape[0])
    ]
    token_load.start()
    for load in loads:
        load.start()
    token_load.wait()
    for send in sends:
        send.start()
    rows, width = held.shape[1:]
    wide[...] = jnp.zeros_like(wide)
    tiles = [None] * TILES
    for j, load in enumerate(loads):
        load.wait()
        wide[:, :width] = held[j]
        first, shift = divmod(j * width, TILE)
        turned = pltpu.roll(wide[...], shift, axis=1) if shift else wide[...]
        for k in range(-(-(width + shift) // TILE)):
            part = turned[:, k * TILE : (k + 1) * TILE]
            old = tiles[first + k]
            tiles[first + k] = part if old is None else old + part
    for j, tile in enumerate(tiles):
        out[j * rows : (j + 1) * rows] = tile.astype(jnp.bfloat16) * LIFT
    for send in sends:
        send.wait()


def pack(tokens, *pieces):
    rows, width = pieces[0].shape
    count = lax.axis_size(RA)
    return pl.pallas_call(
        pack_body,
        in_specs=[HBM] * 7,
        out_specs=[VMEM, HBM],
        out_shape=(
            jax.ShapeDtypeStruct((TILES * rows, TILE), jnp.bfloat16),
            jax.ShapeDtypeStruct((count, *tokens.shape), tokens.dtype),
        ),
        scratch_shapes=[
            pltpu.VMEM((6, rows, width), jnp.float32),
            pltpu.VMEM((rows, WIDE), jnp.float32),
            pltpu.VMEM(tokens.shape, tokens.dtype),
            pltpu.SemaphoreType.DMA((7,)),
            pltpu.SemaphoreType.DMA((count,)),
        ],
    )(*pieces, tokens)


def halves(left, right):
    low = lax.broadcasted_iota(jnp.int32, left.shape, 1) < TILE // 2
    turn = functools.partial(pltpu.roll, shift=TILE // 2, axis=1)
    return jnp.where(low, left, turn(right)), jnp.where(low, turn(left), right)


def to_split(tiles):
    pairs = [halves(*tiles[j : j + 2]) for j in range(0, len(tiles), 2)]
    return [a for a, _ in pairs] + [b for _, b in pairs]


def from_split(tiles):
    count = len(tiles) // 2
    pairs = [halves(tiles[j], tiles[j + count]) for j in range(count)]
    return [tile for pair in pairs for tile in pair]


def tiles_of(value):
    return [value[:, j : j + TILE] for j in range(0, value.shape[1], TILE)]


def split_row(vector):
    rows = jnp.broadcast_to(vector[...], (8, D))
    return jnp.concatenate(to_split(tiles_of(rows)), axis=1)[:1]


def spread_body(pieces, gain, out, own):
    count, rows, _ = pieces.shape
    total = jnp.zeros((rows, 1), jnp.float32)
    for j in range(count):
        piece = pieces[j].astype(jnp.float32)
        total += jnp.sum(piece * piece, axis=1, keepdims=True)
    scale = lax.rsqrt(total / D + EPS)
    few = own.shape[0]
    start = pl.multiple_of(lax.axis_index(RA) * few, few)
    for j in range(0, count, 2):
        normed, kept = [], []
        for i in (j, j + 1):
            value = pieces[i].astype(jnp.float32)
            normed.append(value * scale * gain[:, i * TILE : (i + 1) * TILE])
            kept.append(pieces[i, pl.ds(start, few), :].astype(jnp.float32))
        for side in (0, 1):
            at = slice(side * HALF + j // 2 * TILE, side * HALF + (j // 2 + 1) * TILE)
            out[:, at] = halves(*normed)[side].astype(jnp.bfloat16)
            own[:, at] = halves(*kept)[side]


def spread(pieces, gain):
    count, rows, _ = pieces.shape
    return pl.pallas_call(
        spread_body,
        out_shape=(
            jax.ShapeDtypeStruct((rows, D), jnp.bfloat16),
            jax.ShapeDtypeStruct((rows // count, D), jnp.float32),
        ),
        compiler_params=ROOM,
    )(pieces, gain[None])


def side_by_side(weights, side, first, last):
    groups, _, total, _ = weights.shape
    rows = total // PART
    tiles = [
        weights[:, side, j * rows : (j + 1) * rows, :].reshape(groups * rows, TILE)
        for j in range(first, last)
    ]
    return jnp.concatenate(tiles, axis=1)


def block_body(start, x, s_gate, s_up, *refs):
    parts, (out, scales) = refs[:-2], refs[-2:]
    share = HALF // len(parts)
    places = [
        (part, side, slice(side * HALF + p * share, side * HALF + (p + 1) * share))
        for p, part in enumerate(parts)
        for side in (0, 1)
    ]
    width = s_gate.shape[1]
    scales[...] = jnp.zeros_like(scales)
    scales[0:1, :width] = s_gate[...] / LIFT
    scales[1:2, :width] = s_up[...] / LIFT
    down = (start + 2 * width) // TILE
    place = start + 2 * width - down * TILE
    placed = pltpu.roll(scales[...], place, axis=1)
    across = -(-(start + 2 * width) // TILE)

    both = jnp.zeros((x.shape[0], across * TILE), jnp.float32)
    for part, side, at in places:
        tiles = side_by_side(part, side, 0, across)
        both += jnp.dot(x[:, at], tiles, preferred_element_type=jnp.float32)

    def turned(at):
        return pltpu.roll(both, (place - at) % both.shape[1], axis=1)[:, :WIDE]

    gate = turned(start) * placed[0:1]
    upper = turned(start + width) * placed[1:2]
    hidden = (gate / (1.0 + jnp.exp(-gate)) * upper).astype(jnp.bfloat16)
    for part, side, at in places:
        out[:, at] = lax.dot_general(
            hidden,
            side_by_side(part, side, down, down + WIDE // TILE),
            (((1,), (1,)), ((), ())),
            preferred_element_type=jnp.float32,
        ).astype(jnp.bfloat16)


def block(x, parts, start, s_gate, s_up):
    return pl.pallas_call(
        functools.partial(block_body, start),
        out_shape=jax.ShapeDtypeStruct(x.shape, jnp.bfloat16),
        scratch_shapes=[pltpu.VMEM((8, WIDE), jnp.float32)],
        compiler_params=ROOM,
    )(x, s_gate[None], s_up[None], *parts)


def join_body(last, pieces, before, scale, gain, *outs):
    count = pieces.shape[0]
    added = pieces[0].astype(jnp.float32)
    for j in range(1, count):
        added += pieces[j].astype(jnp.float32)
    values = 0.1 * before[...] + (0.5 / LIFT) * added * split_row(scale)
    meansq = jnp.sum(values * values, axis=1, keepdims=True) / D
    normed = values * lax.rsqrt(meansq + EPS) * split_row(gain)
    if last:
        (out,) = outs
        for j, tile in enumerate(from_split(tiles_of(normed))):
            out[j] = tile.astype(jnp.bfloat16)
    else:
        out, total = outs
        total[...] = values
        for j in range(count):
            out[j] = normed.astype(jnp.bfloat16)


def join(pieces, before, scale, gain, last):
    count, rows, _ = pieces.shape
    shapes = [jax.ShapeDtypeStruct((count, rows, TILE if last else D), jnp.bfloat16)]
    if not last:
        shapes.append(jax.ShapeDtypeStruct((rows, D), jnp.float32))
    return pl.pallas_call(
        functools.partial(join_body, last), out_shape=shapes, compiler_params=ROOM
    )(pieces, before, scale[None], gain[None])


def exchange(pieces):
    return lax.all_to_all(pieces, RA, split_axis=0, concat_axis=0, tiled=True)


def by_rows(partial_value):
    return exchange(partial_value.reshape(lax.axis_size(RA), -1, D))


def in_parts(weights):
    return [part.astype(jnp.bfloat16) for part in jnp.split(weights, 2, axis=0)]


def shards(
    tokens,
    gain_first,
    gate_first,
    gate_first_scale,
    up_first,
    up_first_scale,
    down_first,
    down_first_scale,
    gain_second,
    gate_second,
    gate_second_scale,
    up_second,
    up_second_scale,
    down_second,
    down_second_scale,
    gain_last,
):
    packed, copies = pack(
        tokens, gate_first, up_first, down_first.T, gate_second, up_second, down_second.T
    )
    pieces = exchange(copies)
    packed = packed.reshape(-1).astype(jnp.float16)
    gathered = lax.all_gather(packed, CB, axis=0, tiled=True)
    rows, width = gate_first.shape
    weights = gathered.reshape(-1, 2, TILES * rows, TILE)
    later, start = divmod(3 * width, TILE)
    earlier = in_parts(weights[:, :, : PART * rows])
    normed, own = spread(pieces, gain_first)
    partial_first = block(normed, earlier, 0, gate_first_scale, up_first_scale)
    weights, partial_first = lax.optimization_barrier((weights, partial_first))
    second = in_parts(weights[:, :, later * rows :])
    arrived = by_rows(partial_first)
    copies, first = join(arrived, own, down_first_scale, gain_second, False)
    normed = exchange(copies).reshape(-1, D)
    partial_second = block(normed, second, start, gate_second_scale, up_second_scale)
    (columns,) = join(by_rows(partial_second), first, down_second_scale, gain_last, True)
    return exchange(columns).reshape(tokens.shape)


def solution(mesh):
    torus = Mesh(mesh.devices.reshape(4, 4, 16, 2), ("ra_0", "ra_1", "cb_0", "cb_1"))
    weight, across = P(CB, RA), P(RA, CB)
    return jax.shard_map(
        shards,
        mesh=torus,
        in_specs=(
            P(CB, RA),
            P(),
            weight,
            P(RA),
            weight,
            P(RA),
            across,
            P(),
            P(),
            weight,
            P(RA),
            weight,
            P(RA),
            across,
            P(),
            P(),
        ),
        out_specs=P(CB, RA),
        check_vma=False,
    )
```

```python
import functools

import jax
import jax.numpy as jnp
from jax import lax
from jax.experimental import pallas as pl
from jax.experimental.pallas import tpu as pltpu
from jax.sharding import Mesh
from jax.sharding import PartitionSpec as P


D = 2048
HALF = D // 2
RA = ("ra_0", "ra_1")
CB = ("cb_0", "cb_1")
TILE = 128
TILES = 17
PART = 9
WIDE = 4 * TILE
PARTS = 4
EPS = 1e-06
LIFT = 2.0**18
ROOM = pltpu.CompilerParams(vmem_limit_bytes=20 * 1024 * 1024)
VMEM = pl.BlockSpec(memory_space=pltpu.VMEM)
HBM = pl.BlockSpec(memory_space=pltpu.HBM)


def pack_body(*refs):
    pieces, tokens, out, copies, held, wide, own, sems, copy_sems = refs[:6], *refs[6:]
    loads = [pltpu.make_async_copy(p, held.at[j], sems.at[j]) for j, p in enumerate(pieces)]
    token_load = pltpu.make_async_copy(tokens, own, sems.at[len(pieces)])
    sends = [
        pltpu.make_async_copy(own, copies.at[j], copy_sems.at[j]) for j in range(copies.shape[0])
    ]
    token_load.start()
    for load in loads:
        load.start()
    token_load.wait()
    for send in sends:
        send.start()
    rows, width = held.shape[1:]
    wide[...] = jnp.zeros_like(wide)
    tiles = [None] * TILES
    for j, load in enumerate(loads):
        load.wait()
        wide[:, :width] = held[j]
        first, shift = divmod(j * width, TILE)
        turned = pltpu.roll(wide[...], shift, axis=1) if shift else wide[...]
        for k in range(-(-(width + shift) // TILE)):
            part = turned[:, k * TILE : (k + 1) * TILE]
            old = tiles[first + k]
            tiles[first + k] = part if old is None else old + part
    for j, tile in enumerate(tiles):
        out[j * rows : (j + 1) * rows] = tile.astype(jnp.bfloat16) * LIFT
    for send in sends:
        send.wait()


def pack(tokens, *pieces):
    rows, width = pieces[0].shape
    count = lax.axis_size(RA)
    return pl.pallas_call(
        pack_body,
        in_specs=[HBM] * 7,
        out_specs=[VMEM, HBM],
        out_shape=(
            jax.ShapeDtypeStruct((TILES * rows, TILE), jnp.bfloat16),
            jax.ShapeDtypeStruct((count, *tokens.shape), tokens.dtype),
        ),
        scratch_shapes=[
            pltpu.VMEM((6, rows, width), jnp.float32),
            pltpu.VMEM((rows, WIDE), jnp.float32),
            pltpu.VMEM(tokens.shape, tokens.dtype),
            pltpu.SemaphoreType.DMA((7,)),
            pltpu.SemaphoreType.DMA((count,)),
        ],
    )(*pieces, tokens)


def halves(left, right):
    low = lax.broadcasted_iota(jnp.int32, left.shape, 1) < TILE // 2
    turn = functools.partial(pltpu.roll, shift=TILE // 2, axis=1)
    return jnp.where(low, left, turn(right)), jnp.where(low, turn(left), right)


def to_split(tiles):
    pairs = [halves(*tiles[j : j + 2]) for j in range(0, len(tiles), 2)]
    return [a for a, _ in pairs] + [b for _, b in pairs]


def from_split(tiles):
    count = len(tiles) // 2
    pairs = [halves(tiles[j], tiles[j + count]) for j in range(count)]
    return [tile for pair in pairs for tile in pair]


def tiles_of(value):
    return [value[:, j : j + TILE] for j in range(0, value.shape[1], TILE)]


def split_row(vector):
    rows = jnp.broadcast_to(vector[...], (8, D))
    return jnp.concatenate(to_split(tiles_of(rows)), axis=1)[:1]


def spread_body(pieces, gain, out, own):
    count, rows, _ = pieces.shape
    total = jnp.zeros((rows, 1), jnp.float32)
    for j in range(count):
        piece = pieces[j].astype(jnp.float32)
        total += jnp.sum(piece * piece, axis=1, keepdims=True)
    scale = lax.rsqrt(total / D + EPS)
    few = own.shape[0]
    start = pl.multiple_of(lax.axis_index(RA) * few, few)
    for j in range(0, count, 2):
        normed, kept = [], []
        for i in (j, j + 1):
            value = pieces[i].astype(jnp.float32)
            normed.append(value * scale * gain[:, i * TILE : (i + 1) * TILE])
            kept.append(pieces[i, pl.ds(start, few), :].astype(jnp.float32))
        for side in (0, 1):
            at = slice(side * HALF + j // 2 * TILE, side * HALF + (j // 2 + 1) * TILE)
            out[:, at] = halves(*normed)[side].astype(jnp.bfloat16)
            own[:, at] = halves(*kept)[side]


def spread(pieces, gain):
    count, rows, _ = pieces.shape
    return pl.pallas_call(
        spread_body,
        out_shape=(
            jax.ShapeDtypeStruct((rows, D), jnp.bfloat16),
            jax.ShapeDtypeStruct((rows // count, D), jnp.float32),
        ),
        compiler_params=ROOM,
    )(pieces, gain[None])


def side_by_side(weights, side, first, last):
    groups, _, total, _ = weights.shape
    rows = total // PART
    tiles = [
        weights[:, side, j * rows : (j + 1) * rows, :].reshape(groups * rows, TILE)
        for j in range(first, last)
    ]
    return jnp.concatenate(tiles, axis=1)


def block_body(start, x, s_gate, s_up, *refs):
    parts, (out, scales) = refs[:-2], refs[-2:]
    share = HALF // len(parts)
    places = [
        (part, side, slice(side * HALF + p * share, side * HALF + (p + 1) * share))
        for p, part in enumerate(parts)
        for side in (0, 1)
    ]
    width = s_gate.shape[1]
    scales[...] = jnp.zeros_like(scales)
    scales[0:1, :width] = s_gate[...] / LIFT
    scales[1:2, :width] = s_up[...] / LIFT
    down = (start + 2 * width) // TILE
    place = start + 2 * width - down * TILE
    placed = pltpu.roll(scales[...], place, axis=1)
    across = -(-(start + 2 * width) // TILE)

    both = jnp.zeros((x.shape[0], across * TILE), jnp.float32)
    for part, side, at in places:
        tiles = side_by_side(part, side, 0, across)
        both += jnp.dot(x[:, at], tiles, preferred_element_type=jnp.float32)

    def turned(at):
        return pltpu.roll(both, (place - at) % both.shape[1], axis=1)[:, :WIDE]

    gate = turned(start) * placed[0:1]
    upper = turned(start + width) * placed[1:2]
    hidden = (gate / (1.0 + jnp.exp(-gate)) * upper).astype(jnp.bfloat16)
    for part, side, at in places:
        out[:, at] = lax.dot_general(
            hidden,
            side_by_side(part, side, down, down + WIDE // TILE),
            (((1,), (1,)), ((), ())),
            preferred_element_type=jnp.float32,
        ).astype(jnp.bfloat16)


def block(x, parts, start, s_gate, s_up):
    return pl.pallas_call(
        functools.partial(block_body, start),
        out_shape=jax.ShapeDtypeStruct(x.shape, jnp.bfloat16),
        scratch_shapes=[pltpu.VMEM((8, WIDE), jnp.float32)],
        compiler_params=ROOM,
    )(x, s_gate[None], s_up[None], *parts)


def join_body(last, pieces, before, scale, gain, *outs):
    count = pieces.shape[0]
    added = pieces[0].astype(jnp.float32)
    for j in range(1, count):
        added += pieces[j].astype(jnp.float32)
    values = 0.1 * before[...] + (0.5 / LIFT) * added * split_row(scale)
    meansq = jnp.sum(values * values, axis=1, keepdims=True) / D
    normed = values * lax.rsqrt(meansq + EPS) * split_row(gain)
    if last:
        (out,) = outs
        for j, tile in enumerate(from_split(tiles_of(normed))):
            out[j] = tile.astype(jnp.bfloat16)
    else:
        out, total = outs
        total[...] = values
        for j in range(count):
            out[j] = normed.astype(jnp.bfloat16)


def join(pieces, before, scale, gain, last):
    count, rows, _ = pieces.shape
    shapes = [jax.ShapeDtypeStruct((count, rows, TILE if last else D), jnp.bfloat16)]
    if not last:
        shapes.append(jax.ShapeDtypeStruct((rows, D), jnp.float32))
    return pl.pallas_call(
        functools.partial(join_body, last), out_shape=shapes, compiler_params=ROOM
    )(pieces, before, scale[None], gain[None])


def exchange(pieces):
    return lax.all_to_all(pieces, RA, split_axis=0, concat_axis=0, tiled=True)


def by_rows(partial_value):
    return exchange(partial_value.reshape(lax.axis_size(RA), -1, D))


def in_parts(weights):
    parts, count = [], PARTS
    size = weights.shape[0] // count
    for j in range(count):
        part = weights[j * size : (j + 1) * size].astype(jnp.bfloat16)
        weights, part = lax.optimization_barrier((weights, part))
        parts.append(part)
    return parts


def shards(
    tokens,
    gain_first,
    gate_first,
    gate_first_scale,
    up_first,
    up_first_scale,
    down_first,
    down_first_scale,
    gain_second,
    gate_second,
    gate_second_scale,
    up_second,
    up_second_scale,
    down_second,
    down_second_scale,
    gain_last,
):
    packed, copies = pack(
        tokens, gate_first, up_first, down_first.T, gate_second, up_second, down_second.T
    )
    pieces = exchange(copies)
    packed = packed.reshape(-1).astype(jnp.float16)
    gathered = lax.all_gather(packed, CB, axis=0, tiled=True)
    rows, width = gate_first.shape
    weights = gathered.reshape(-1, 2, TILES * rows, TILE)
    later, start = divmod(3 * width, TILE)
    earlier = in_parts(weights[:, :, : PART * rows])
    normed, own = spread(pieces, gain_first)
    partial_first = block(normed, earlier, 0, gate_first_scale, up_first_scale)
    weights, partial_first = lax.optimization_barrier((weights, partial_first))
    second = in_parts(weights[:, :, later * rows :])
    arrived = by_rows(partial_first)
    copies, first = join(arrived, own, down_first_scale, gain_second, False)
    normed = exchange(copies).reshape(-1, D)
    partial_second = block(normed, second, start, gate_second_scale, up_second_scale)
    (columns,) = join(by_rows(partial_second), first, down_second_scale, gain_last, True)
    return exchange(columns).reshape(tokens.shape)


def solution(mesh):
    torus = Mesh(mesh.devices.reshape(4, 4, 16, 2), ("ra_0", "ra_1", "cb_0", "cb_1"))
    weight, across = P(CB, RA), P(RA, CB)
    return jax.shard_map(
        shards,
        mesh=torus,
        in_specs=(
            P(CB, RA),
            P(),
            weight,
            P(RA),
            weight,
            P(RA),
            across,
            P(),
            P(),
            weight,
            P(RA),
            weight,
            P(RA),
            across,
            P(),
            P(),
        ),
        out_specs=P(CB, RA),
        check_vma=False,
    )
```

```python
import functools

import jax
import jax.numpy as jnp
from jax import lax
from jax.experimental import pallas as pl
from jax.experimental.pallas import tpu as pltpu
from jax.sharding import Mesh
from jax.sharding import PartitionSpec as P


D = 2048
HALF = D // 2
RA = ("ra_0", "ra_1")
CB = ("cb_0", "cb_1")
TILE = 128
TILES = 17
PART = 9
WIDE = 4 * TILE
CUT = 4
EPS = 1e-06
LIFT = 2.0**18
ROOM = pltpu.CompilerParams(vmem_limit_bytes=20 * 1024 * 1024)
VMEM = pl.BlockSpec(memory_space=pltpu.VMEM)
HBM = pl.BlockSpec(memory_space=pltpu.HBM)


def pack_body(*refs):
    pieces, tokens, out, copies, held, wide, own, sems, copy_sems = refs[:6], *refs[6:]
    loads = [pltpu.make_async_copy(p, held.at[j], sems.at[j]) for j, p in enumerate(pieces)]
    token_load = pltpu.make_async_copy(tokens, own, sems.at[len(pieces)])
    sends = [
        pltpu.make_async_copy(own, copies.at[j], copy_sems.at[j]) for j in range(copies.shape[0])
    ]
    token_load.start()
    for load in loads:
        load.start()
    token_load.wait()
    for send in sends:
        send.start()
    rows, width = held.shape[1:]
    wide[...] = jnp.zeros_like(wide)
    tiles = [None] * TILES
    for j, load in enumerate(loads):
        load.wait()
        wide[:, :width] = held[j]
        first, shift = divmod(j * width, TILE)
        turned = pltpu.roll(wide[...], shift, axis=1) if shift else wide[...]
        for k in range(-(-(width + shift) // TILE)):
            part = turned[:, k * TILE : (k + 1) * TILE]
            old = tiles[first + k]
            tiles[first + k] = part if old is None else old + part
    for j, tile in enumerate(tiles):
        out[j * rows : (j + 1) * rows] = tile.astype(jnp.bfloat16) * LIFT
    for send in sends:
        send.wait()


def pack(tokens, *pieces):
    rows, width = pieces[0].shape
    count = lax.axis_size(RA)
    return pl.pallas_call(
        pack_body,
        in_specs=[HBM] * 7,
        out_specs=[VMEM, HBM],
        out_shape=(
            jax.ShapeDtypeStruct((TILES * rows, TILE), jnp.bfloat16),
            jax.ShapeDtypeStruct((count, *tokens.shape), tokens.dtype),
        ),
        scratch_shapes=[
            pltpu.VMEM((6, rows, width), jnp.float32),
            pltpu.VMEM((rows, WIDE), jnp.float32),
            pltpu.VMEM(tokens.shape, tokens.dtype),
            pltpu.SemaphoreType.DMA((7,)),
            pltpu.SemaphoreType.DMA((count,)),
        ],
    )(*pieces, tokens)


def halves(left, right):
    low = lax.broadcasted_iota(jnp.int32, left.shape, 1) < TILE // 2
    turn = functools.partial(pltpu.roll, shift=TILE // 2, axis=1)
    return jnp.where(low, left, turn(right)), jnp.where(low, turn(left), right)


def to_split(tiles):
    pairs = [halves(*tiles[j : j + 2]) for j in range(0, len(tiles), 2)]
    return [a for a, _ in pairs] + [b for _, b in pairs]


def from_split(tiles):
    count = len(tiles) // 2
    pairs = [halves(tiles[j], tiles[j + count]) for j in range(count)]
    return [tile for pair in pairs for tile in pair]


def tiles_of(value):
    return [value[:, j : j + TILE] for j in range(0, value.shape[1], TILE)]


def split_row(vector):
    rows = jnp.broadcast_to(vector[...], (8, D))
    return jnp.concatenate(to_split(tiles_of(rows)), axis=1)[:1]


def spread_body(pieces, gain, out, own):
    count, rows, _ = pieces.shape
    total = jnp.zeros((rows, 1), jnp.float32)
    for j in range(count):
        piece = pieces[j].astype(jnp.float32)
        total += jnp.sum(piece * piece, axis=1, keepdims=True)
    scale = lax.rsqrt(total / D + EPS)
    few = own.shape[0]
    start = pl.multiple_of(lax.axis_index(RA) * few, few)
    for j in range(0, count, 2):
        normed, kept = [], []
        for i in (j, j + 1):
            value = pieces[i].astype(jnp.float32)
            normed.append(value * scale * gain[:, i * TILE : (i + 1) * TILE])
            kept.append(pieces[i, pl.ds(start, few), :].astype(jnp.float32))
        for side in (0, 1):
            at = slice(side * HALF + j // 2 * TILE, side * HALF + (j // 2 + 1) * TILE)
            out[:, at] = halves(*normed)[side].astype(jnp.bfloat16)
            own[:, at] = halves(*kept)[side]


def spread(pieces, gain):
    count, rows, _ = pieces.shape
    return pl.pallas_call(
        spread_body,
        out_shape=(
            jax.ShapeDtypeStruct((rows, D), jnp.bfloat16),
            jax.ShapeDtypeStruct((rows // count, D), jnp.float32),
        ),
        compiler_params=ROOM,
    )(pieces, gain[None])


def side_by_side(weights, side, first, last):
    groups, _, total, _ = weights.shape
    rows = total // PART
    tiles = [
        weights[:, side, j * rows : (j + 1) * rows, :].reshape(groups * rows, TILE)
        for j in range(first, last)
    ]
    return jnp.concatenate(tiles, axis=1)


def block_body(start, x, s_gate, s_up, *refs):
    parts, (out, scales) = refs[:-2], refs[-2:]
    ends = [0]
    for part in parts:
        ends.append(ends[-1] + part.shape[0] * part.shape[2] // PART)
    places = [
        (part, side, slice(side * HALF + ends[p], side * HALF + ends[p + 1]))
        for p, part in enumerate(parts)
        for side in (0, 1)
    ]
    width = s_gate.shape[1]
    scales[...] = jnp.zeros_like(scales)
    scales[0:1, :width] = s_gate[...] / LIFT
    scales[1:2, :width] = s_up[...] / LIFT
    down = (start + 2 * width) // TILE
    place = start + 2 * width - down * TILE
    placed = pltpu.roll(scales[...], place, axis=1)
    across = -(-(start + 2 * width) // TILE)

    both = jnp.zeros((x.shape[0], across * TILE), jnp.float32)
    for part, side, at in places:
        tiles = side_by_side(part, side, 0, across)
        both += jnp.dot(x[:, at], tiles, preferred_element_type=jnp.float32)

    def turned(at):
        return pltpu.roll(both, (place - at) % both.shape[1], axis=1)[:, :WIDE]

    gate = turned(start) * placed[0:1]
    upper = turned(start + width) * placed[1:2]
    hidden = (gate / (1.0 + jnp.exp(-gate)) * upper).astype(jnp.bfloat16)
    for part, side, at in places:
        out[:, at] = lax.dot_general(
            hidden,
            side_by_side(part, side, down, down + WIDE // TILE),
            (((1,), (1,)), ((), ())),
            preferred_element_type=jnp.float32,
        ).astype(jnp.bfloat16)


def block(x, parts, start, s_gate, s_up):
    return pl.pallas_call(
        functools.partial(block_body, start),
        out_shape=jax.ShapeDtypeStruct(x.shape, jnp.bfloat16),
        scratch_shapes=[pltpu.VMEM((8, WIDE), jnp.float32)],
        compiler_params=ROOM,
    )(x, s_gate[None], s_up[None], *parts)


def join_body(last, pieces, before, scale, gain, *outs):
    count = pieces.shape[0]
    added = pieces[0].astype(jnp.float32)
    for j in range(1, count):
        added += pieces[j].astype(jnp.float32)
    values = 0.1 * before[...] + (0.5 / LIFT) * added * split_row(scale)
    meansq = jnp.sum(values * values, axis=1, keepdims=True) / D
    normed = values * lax.rsqrt(meansq + EPS) * split_row(gain)
    if last:
        (out,) = outs
        for j, tile in enumerate(from_split(tiles_of(normed))):
            out[j] = tile.astype(jnp.bfloat16)
    else:
        out, total = outs
        total[...] = values
        for j in range(count):
            out[j] = normed.astype(jnp.bfloat16)


def join(pieces, before, scale, gain, last):
    count, rows, _ = pieces.shape
    shapes = [jax.ShapeDtypeStruct((count, rows, TILE if last else D), jnp.bfloat16)]
    if not last:
        shapes.append(jax.ShapeDtypeStruct((rows, D), jnp.float32))
    return pl.pallas_call(
        functools.partial(join_body, last), out_shape=shapes, compiler_params=ROOM
    )(pieces, before, scale[None], gain[None])


def exchange(pieces):
    return lax.all_to_all(pieces, RA, split_axis=0, concat_axis=0, tiled=True)


def by_rows(partial_value):
    return exchange(partial_value.reshape(lax.axis_size(RA), -1, D))


def in_parts(weights):
    return [part.astype(jnp.bfloat16) for part in jnp.split(weights, [CUT], axis=0)]


def shards(
    tokens,
    gain_first,
    gate_first,
    gate_first_scale,
    up_first,
    up_first_scale,
    down_first,
    down_first_scale,
    gain_second,
    gate_second,
    gate_second_scale,
    up_second,
    up_second_scale,
    down_second,
    down_second_scale,
    gain_last,
):
    packed, copies = pack(
        tokens, gate_first, up_first, down_first.T, gate_second, up_second, down_second.T
    )
    pieces = exchange(copies)
    packed = packed.reshape(-1).astype(jnp.float16)
    gathered = lax.all_gather(packed, CB, axis=0, tiled=True)
    rows, width = gate_first.shape
    weights = gathered.reshape(-1, 2, TILES * rows, TILE)
    later, start = divmod(3 * width, TILE)
    earlier = in_parts(weights[:, :, : PART * rows])
    normed, own = spread(pieces, gain_first)
    partial_first = block(normed, earlier, 0, gate_first_scale, up_first_scale)
    weights, partial_first = lax.optimization_barrier((weights, partial_first))
    second = in_parts(weights[:, :, later * rows :])
    arrived = by_rows(partial_first)
    copies, first = join(arrived, own, down_first_scale, gain_second, False)
    normed = exchange(copies).reshape(-1, D)
    partial_second = block(normed, second, start, gate_second_scale, up_second_scale)
    (columns,) = join(by_rows(partial_second), first, down_second_scale, gain_last, True)
    return exchange(columns).reshape(tokens.shape)


def solution(mesh):
    torus = Mesh(mesh.devices.reshape(4, 4, 16, 2), ("ra_0", "ra_1", "cb_0", "cb_1"))
    weight, across = P(CB, RA), P(RA, CB)
    return jax.shard_map(
        shards,
        mesh=torus,
        in_specs=(
            P(CB, RA),
            P(),
            weight,
            P(RA),
            weight,
            P(RA),
            across,
            P(),
            P(),
            weight,
            P(RA),
            weight,
            P(RA),
            across,
            P(),
            P(),
        ),
        out_specs=P(CB, RA),
        check_vma=False,
    )
```
